32 devices in a mesh: grp: 2 (over y), tp: 4 (over z), dp: 4 (over x, core).
Axes of the slice: x: 2, y: 2, z: 4, core: 2. Of those that a mesh axis runs over, the one named last changes fastest.
Arguments:
- tokens: bfloat16 [64, 8, 4096], P(('grp', 'tp'), None, 'dp'), parts along dimension 0, may hold values from -6 to 6
- lengths: int32 [64], P('grp'), parts along dimension 0, may hold values from 1 to 8, 112 in all
- norm_gain: float32 [2, 4096], P(None, 'dp'), may hold values from 0.1 to 1.9
- w_recept: bfloat16 [2, 4096, 2048], P(None, 'dp', 'tp'), may hold values from -0.09375 to 0.09375
- w_key: bfloat16 [2, 4096, 2048], P(None, 'dp', 'tp'), may hold values from -0.09375 to 0.09375
- w_value: bfloat16 [2, 4096, 2048], P(None, 'dp', 'tp'), may hold values from -0.09375 to 0.09375
- w_decay: bfloat16 [2, 4096, 2048], P(None, 'dp', 'tp'), may hold values from -0.375 to 0.375
- w_rate: bfloat16 [2, 4096, 2048], P(None, 'dp', 'tp'), may hold values from -0.09375 to 0.09375
- w_gate: bfloat16 [2, 4096, 2048], P(None, 'dp', 'tp'), may hold values from -0.09375 to 0.09375
- w_out: bfloat16 [2, 2048, 4096], P(None, 'tp', 'dp'), may hold values from -0.125 to 0.125
- decay_base: float32 [2, 2048], P(None, 'tp'), may hold values from -4 to 3
- out_gain: float32 [2, 2048], P(None, 'tp'), may hold values from 0.1 to 1.9
- states: float32 [2, 64, 64, 2048], P(None, ('grp', 'dp'), None, 'tp'), parts along dimension 1, may hold values from -6 to 6
Outputs:
- stream_out: float32 [64, 8, 4096], P(('grp', 'tp'), None, 'dp'), parts along dimension 0
- new_states: float32 [2, 64, 64, 2048], P(None, ('grp', 'dp'), None, 'tp'), parts along dimension 1
The draws below stay inside these ranges and needn't reach their ends.
There are 2 independent parts, one for each index of `grp`. The reference program is written for one: setup_inputs(seed, part) draws one part's arguments, and reference() takes and returns one part's arrays. A program takes and returns all parts, laid end to end along the dimension named above; an argument that names none is the same for every part. Nothing has to cross between parts.
Inputs may be any that keep to these rules, and one draw needn't show every extreme that they name: lengths[b] first tokens of sequence b are live; together they count 7 * 16 and the largest is 8.
All inputs are finite; a program needn't handle non-finite values.
Results may differ from the reference program's by a relative error of at most 0.0061.
Values may be sent and summed in bfloat16 or wider, within the bound.
A program may use at most 128 MiB of HBM per device.

```python
import math
import jax
import jax.numpy as jnp
import numpy as np
from jax import lax

D = 4096
HEAD = 64
WIDTH = 2048
STEPS = 8
BLOCKS = 2
SEQS = 32


def draw_tokens(key, part):
    row_key, column_key, value_key = jax.random.split(key, 3)
    rising = jnp.exp(jnp.linspace(math.log(0.5), math.log(2.0), D))
    rough = jax.random.uniform(column_key, (D,), jnp.float32, 0.6, 1.5)
    row_scale = jnp.exp(jax.random.uniform(row_key, (SEQS, STEPS, 1), jnp.float32, math.log(0.1), math.log(1.0)))
    values = jax.random.normal(value_key, (SEQS, STEPS, D), jnp.float32)
    drawn = jnp.clip(values * row_scale * rising * rough, -6.0, 6.0)
    return drawn.astype(jnp.bfloat16)


def steps_of(key, shape, shards, least, high):
    def one(dim, parts):
        heights = jax.random.uniform(jax.random.fold_in(jax.random.fold_in(key, 6), dim), (parts,), jnp.float32, least / len(shards), high / len(shards))
        return jnp.repeat(jnp.exp(heights), shape[dim] // parts).reshape((-1,) + (1,) * (len(shape) - dim - 1))

    level = one(*shards[0])
    for cut in shards[1:]:
        level = level * one(*cut)
    return level


def length_profile(count, total, bound, skew):
    weights = [(1 << 20) // math.isqrt(grade ** skew) + 1 for grade in range(2, count + 1)]
    surplus, given = total - bound - (count - 1), [1] * (count - 1)
    while surplus > 0:
        movable = [i for i in range(count - 1) if given[i] < bound]
        whole, budget = sum([weights[i] for i in movable]), surplus
        for i in movable:
            extra = min(bound - given[i], max(1, budget * weights[i] // whole), surplus)
            given[i] = given[i] + extra
            surplus = surplus - extra
    return np.array([bound] + given)


def ragged_sizes(stream_key, number_of, total, most, skew):
    if number_of == 2:
        one = jax.random.randint(stream_key, (), max(1, total - most), min(most, total - 1) + 1)
        return jnp.stack([one, total - one])
    tallies = jnp.asarray(length_profile(number_of, total, most, skew), jnp.int32)
    twos = (number_of - 1) // 2
    donor, taker = tallies[1:1 + 2 * twos:2], tallies[2:2 + 2 * twos:2]
    margin = jnp.minimum(donor - 1, most - taker)
    moved = jax.random.randint(jax.random.fold_in(stream_key, 1), (twos,), 0, 1 << 20) % (margin + 1)
    tallies = tallies.at[1:1 + 2 * twos:2].set(donor - moved).at[2:2 + 2 * twos:2].set(taker + moved)
    return tallies[jax.random.permutation(jax.random.fold_in(stream_key, 2), number_of)]


def bell_draw(own_key, shape, deviation, reach, pieces=(), kind=jnp.bfloat16):
    gain = steps_of(own_key, shape, pieces, -0.22, 0.18) if pieces else 1.0
    array = jax.random.normal(own_key, shape, jnp.float32) * deviation * gain
    return jnp.minimum(jnp.maximum(array, -reach), reach).astype(kind)


def setup_inputs(seed: int = 0, part: int = 0) -> dict:
    arg_keys = jax.random.split(jax.random.key(seed), 14)
    part_splits = jax.random.split(jax.random.fold_in(arg_keys[13], part), 14)
    tokens = draw_tokens(jax.random.fold_in(jax.random.fold_in(arg_keys[13], part), 71), part)
    lengths = ragged_sizes(part_splits[1], SEQS, 7 * SEQS // 2, STEPS, 2).astype(jnp.int32)
    norm_gain = jnp.clip(1.0 + 0.18 * jax.random.normal(arg_keys[2], (BLOCKS, D), jnp.float32), 0.1, 1.9)
    w_recept = bell_draw(arg_keys[3], (BLOCKS, D, WIDTH), D ** -0.5, 0.09375, ((1, 4), (2, 4)))
    w_key = bell_draw(arg_keys[4], (BLOCKS, D, WIDTH), D ** -0.5, 0.09375, ((1, 4), (2, 4)))
    w_value = bell_draw(arg_keys[5], (BLOCKS, D, WIDTH), D ** -0.5, 0.09375, ((1, 4), (2, 4)))
    w_decay = bell_draw(arg_keys[6], (BLOCKS, D, WIDTH), (D // 16) ** -0.5, 0.375, ((1, 4), (2, 4)))
    w_rate = bell_draw(arg_keys[7], (BLOCKS, D, WIDTH), D ** -0.5, 0.09375, ((1, 4), (2, 4)))
    w_gate = bell_draw(arg_keys[8], (BLOCKS, D, WIDTH), D ** -0.5, 0.09375, ((1, 4), (2, 4)))
    w_out = bell_draw(arg_keys[9], (BLOCKS, WIDTH, D), WIDTH ** -0.5, 0.125, ((1, 4), (2, 4)))
    decay_base = jnp.clip(-4.0 + 7.0 * jax.random.uniform(arg_keys[10], (BLOCKS, WIDTH), jnp.float32) ** steps_of(arg_keys[10], (BLOCKS, WIDTH), ((1, 4),), -0.2, 0.2), -4.0, 3.0)
    out_gain = jnp.clip(1.0 + 0.18 * jax.random.normal(arg_keys[11], (BLOCKS, WIDTH), jnp.float32), 0.1, 1.9)
    states = bell_draw(part_splits[12], (BLOCKS, SEQS, HEAD, WIDTH), 1.0, 6.0, ((1, 4), (3, 4)), jnp.float32)
    return {"tokens": tokens, "lengths": lengths, "norm_gain": norm_gain, "w_recept": w_recept, "w_key": w_key, "w_value": w_value, "w_decay": w_decay, "w_rate": w_rate, "w_gate": w_gate, "w_out": w_out, "decay_base": decay_base, "out_gain": out_gain, "states": states}


group_eps = 0.00064
norm_eps = 1e-06
key_eps = 1e-06
decay_scale = 0.606531
highest = lax.Precision.HIGHEST

def mix_heads(state_in, recept, keys_in, values, decay_pre, rate_pre, gate_pre, base_shift, out_scale, live_mask, head_size):
    row_count, step_count, width_all = recept.shape
    head_count = width_all // head_size
    shape_heads = (row_count, step_count, head_count, head_size)
    decay_rate = jnp.exp(-decay_scale * jax.nn.sigmoid(decay_pre + base_shift)).reshape(shape_heads)
    learn_rate = jax.nn.sigmoid(rate_pre).reshape(shape_heads)
    key_heads = keys_in.reshape(shape_heads)
    unit_keys = key_heads * lax.rsqrt(lax.optimization_barrier(jnp.sum(key_heads * key_heads, axis=3, keepdims=True)) + key_eps)
    removal = unit_keys * learn_rate
    recept_heads = recept.reshape(shape_heads)
    value_heads = values.reshape(shape_heads)
    memory = state_in.reshape(row_count, head_size, head_count, head_size)
    outputs = []
    for position in range(step_count):
        seen_part = jnp.einsum('bihj,bhj->bhi', memory, unit_keys[:, position], precision=highest)
        updated = memory * decay_rate[:, position][:, None, :, :] - jnp.swapaxes(seen_part, 1, 2)[:, :, :, None] * removal[:, position][:, None, :, :] + jnp.swapaxes(value_heads[:, position], 1, 2)[:, :, :, None] * key_heads[:, position][:, None, :, :]
        memory = jnp.where(live_mask[:, position][:, None, None, None], updated, memory)
        outputs.append(jnp.einsum('bihj,bhj->bhi', memory, recept_heads[:, position], precision=highest))
    readout = jnp.stack(outputs, axis=1)
    centered = readout - lax.optimization_barrier(jnp.mean(readout, axis=3, keepdims=True))
    normed = centered * lax.rsqrt(lax.optimization_barrier(jnp.mean(centered * centered, axis=3, keepdims=True)) + group_eps)
    gated = normed.reshape(row_count, step_count, width_all) * out_scale * jax.nn.sigmoid(gate_pre)
    gated = jnp.where(live_mask[:, :, None], gated, 0.0)
    return (gated.astype(jnp.bfloat16), memory.reshape(row_count, head_size, width_all))

def reference(tokens, lengths, norm_gain, w_recept, w_key, w_value, w_decay, w_rate, w_gate, w_out, decay_base, out_gain, states):
    live_mask = jnp.arange(STEPS, dtype=jnp.int32)[None, :] < lengths[:, None]
    current = tokens.astype(jnp.float32)
    finals = []
    for block_index in range(BLOCKS):
        inv_rms = lax.rsqrt(lax.optimization_barrier(jnp.sum(current * current, axis=2)) / D + norm_eps)
        scaled = (current * norm_gain[block_index]).astype(jnp.bfloat16).reshape(SEQS * STEPS, D)
        projected = [jnp.dot(scaled, weight[block_index], preferred_element_type=jnp.float32).reshape(SEQS, STEPS, WIDTH) * inv_rms[:, :, None] for weight in (w_recept, w_key, w_value, w_decay, w_rate, w_gate)]
        gated, final_state = mix_heads(states[block_index], projected[0], projected[1], projected[2], projected[3], projected[4], projected[5], decay_base[block_index], out_gain[block_index], live_mask, HEAD)
        finals.append(final_state)
        output = jnp.dot(gated.reshape(SEQS * STEPS, WIDTH), w_out[block_index], preferred_element_type=jnp.float32).reshape(SEQS, STEPS, D)
        current = current + output
    return (current, jnp.stack(finals, axis=0))
```

```python
import functools

import jax
import jax.numpy as jnp
from jax import lax
from jax.experimental import pallas as pl
from jax.experimental.pallas import tpu as pltpu
from jax.sharding import PartitionSpec as P

HEAD = 64
BLOCKS = 2
LANES = 128
CORES = 2

group_eps = 0.00064
norm_eps = 1e-06
key_eps = 1e-06
decay_scale = 0.606531
MESH = pl.DeviceIdType.MESH
F32 = jnp.float32
BF16 = jnp.bfloat16


def remote(src, dst, send, recv, axis, peer):
    return pltpu.make_async_remote_copy(
        src_ref=src,
        dst_ref=dst,
        send_sem=send,
        recv_sem=recv,
        device_id={axis: peer},
        device_id_type=MESH,
    )


def greet(peers):
    barrier = pltpu.get_barrier_semaphore()
    for axis, peer in peers:
        pl.semaphore_signal(barrier, inc=1, device_id={axis: peer}, device_id_type=MESH)
    pl.semaphore_wait(barrier, len(peers))


def project_kernel(
    block, ntp, ndp, rows, width,
    x_ref, gain_ref, w0, w1, w2, w3, w4, w5,
    out_ref, total_ref,
    wbuf, xg, sqg, part, send_a, recv_a, send_b, recv_b, sq_a, sq_ra, sq_b, sq_rb,
    wsem, xs_sem, xr_sem, ss_sem, sr_sem, as_sem, ar_sem, bs_sem, br_sem,
    qas_sem, qar_sem, qbs_sem, qbr_sem,
):
    weights = (w0, w1, w2, w3, w4, w5)
    chunks, depth, _ = wbuf.shape
    halves = chunks // 6
    nx = ndp // CORES
    tp = lax.axis_index("tp")
    dp = lax.axis_index("dp")
    core = lax.rem(dp, CORES)
    xpos = dp // CORES
    partner = dp + 1 - 2 * core

    def load(c):
        return pltpu.make_async_copy(
            weights[c // halves].at[block, :, pl.ds((c % halves) * width, width)],
            wbuf.at[c],
            wsem.at[c],
        )

    for c in range(chunks):
        load(c).start()
    x = x_ref[...].astype(F32)
    xg[tp] = (x * gain_ref[...]).astype(BF16)
    sq = x * x
    acc = sq[:, 0:LANES]
    for k in range(1, depth // LANES):
        acc = acc + sq[:, k * LANES : (k + 1) * LANES]
    sqg[tp] = acc
    peers = [("tp", lax.rem(tp + k, ntp)) for k in range(1, ntp)]
    peers += [("dp", partner)]
    peers += [("dp", CORES * lax.rem(xpos + k, nx) + core) for k in range(1, nx)]
    greet(peers)

    gathers = []
    for k in range(1, ntp):
        peer = lax.rem(tp + k, ntp)
        cp = remote(xg.at[tp], xg.at[tp], xs_sem.at[k], xr_sem.at[k], "tp", peer)
        cq = remote(sqg.at[tp], sqg.at[tp], ss_sem.at[k], sr_sem.at[k], "tp", peer)
        cp.start()
        cq.start()
        gathers += [cp, cq]
    for k in range(1, ntp):
        src = lax.rem(tp + ntp - k, ntp)
        remote(xg.at[src], xg.at[src], xs_sem.at[k], xr_sem.at[k], "tp", src).wait_recv()
        remote(sqg.at[src], sqg.at[src], ss_sem.at[k], sr_sem.at[k], "tp", src).wait_recv()

    sq_all = sqg[...].reshape(ndp, rows, LANES)
    part_sq = [sq_all[d] for d in range(ndp)]

    def pick(parts, x_at, which):
        return jnp.where(which == 0, parts[CORES * x_at], parts[CORES * x_at + 1])

    for xd in range(nx):
        sq_a[xd] = pick(part_sq, xd, 1 - core)
        sq_b[xd] = pick(part_sq, xd, core)
    copy_qa = remote(sq_a, sq_ra, qas_sem, qar_sem, "dp", partner)
    copy_qa.start()

    def copy_a(c):
        return remote(send_a.at[c], recv_a.at[c], as_sem.at[c], ar_sem.at[c], "dp", partner)

    def copy_b(c, k):
        xd = lax.rem(xpos + k, nx)
        return remote(
            send_b.at[c, k], recv_b.at[c, k], bs_sem.at[c, k], br_sem.at[c, k],
            "dp", CORES * xd + core,
        )

    def stage_b(c):
        copy_a(c).wait_recv()
        for k in range(1, nx):
            xd = lax.rem(xpos + k, nx)
            send_b[c, k] = (part[c, CORES * xd + core] + recv_a[c, xd].astype(F32)).astype(BF16)
            copy_b(c, k).start()

    def first(c, carry):
        pltpu.make_async_copy(wbuf.at[c], wbuf.at[c], wsem.at[c]).wait()
        res = jnp.dot(
            xg[...].reshape(ndp * rows, depth), wbuf[c], preferred_element_type=F32
        )
        part[c] = res.reshape(ndp, rows, width)
        for xd in range(nx):
            send_a[c, xd] = part[c, CORES * xd + 1 - core].astype(BF16)
        copy_a(c).start()

        @pl.when(c > 0)
        def _():
            stage_b(c - 1)

        return carry

    lax.fori_loop(0, chunks, first, 0)
    copy_qa.wait_recv()
    for xd in range(nx):
        sq_b[xd] = sq_b[xd] + sq_ra[xd]
    qb = []
    for k in range(1, nx):
        xd = lax.rem(xpos + k, nx)
        cp = remote(
            sq_b.at[xd], sq_rb.at[k], qbs_sem.at[k], qbr_sem.at[k], "dp", CORES * xd + core
        )
        cp.start()
        qb.append(cp)
    stage_b(chunks - 1)

    def last(c, carry):
        own = part[c, CORES * xpos + core] + recv_a[c, xpos].astype(F32)
        for k in range(1, nx):
            copy_b(c, k).wait_recv()
            own = own + recv_b[c, k].astype(F32)
        out_ref[:, pl.ds(pl.multiple_of(c * width, width), width)] = own
        copy_a(c).wait_send()
        for k in range(1, nx):
            copy_b(c, k).wait_send()
        return carry

    lax.fori_loop(0, chunks, last, 0)
    total = sq_b[xpos]
    for k in range(1, nx):
        qb[k - 1].wait_recv()
        total = total + sq_rb[k]
    total_ref[...] = total
    copy_qa.wait_send()
    for cp in qb:
        cp.wait_send()
    for cp in gathers:
        cp.wait_send()


def project(block, ntp, ndp, rows, x, gain, weights, ident):
    here, depth = x.shape
    span = weights[0].shape[2]
    width = min(256, span)
    chunks = 6 * span // width
    nx = ndp // CORES
    dma = pltpu.SemaphoreType.DMA
    vmem = pl.BlockSpec(memory_space=pltpu.VMEM)
    hbm = pl.BlockSpec(memory_space=pl.ANY)
    return pl.pallas_call(
        functools.partial(project_kernel, block, ntp, ndp, rows, width),
        out_shape=(
            jax.ShapeDtypeStruct((rows, 6 * span), F32),
            jax.ShapeDtypeStruct((rows, LANES), F32),
        ),
        in_specs=[vmem, vmem] + [hbm] * 6,
        out_specs=(vmem, vmem),
        scratch_shapes=[
            pltpu.VMEM((chunks, depth, width), BF16),
            pltpu.VMEM((ntp, here, depth), BF16),
            pltpu.VMEM((ntp, here, LANES), F32),
            pltpu.VMEM((chunks, ndp, rows, width), F32),
            pltpu.VMEM((chunks, nx, rows, width), BF16),
            pltpu.VMEM((chunks, nx, rows, width), BF16),
            pltpu.VMEM((chunks, nx, rows, width), BF16),
            pltpu.VMEM((chunks, nx, rows, width), BF16),
            pltpu.VMEM((nx, rows, LANES), F32),
            pltpu.VMEM((nx, rows, LANES), F32),
            pltpu.VMEM((nx, rows, LANES), F32),
            pltpu.VMEM((nx, rows, LANES), F32),
            dma((chunks,)),
            dma((ntp,)), dma((ntp,)), dma((ntp,)), dma((ntp,)),
            dma((chunks,)), dma((chunks,)),
            dma((chunks, nx)), dma((chunks, nx)),
            dma, dma, dma((nx,)), dma((nx,)),
        ],
        compiler_params=pltpu.CompilerParams(
            collective_id=ident, has_side_effects=True, vmem_limit_bytes=48 * 1024 * 1024
        ),
        name="project%d" % block,
    )(x, gain, *weights)


def split_dot(a, b):
    hi = a.astype(BF16)
    lo = (a - hi.astype(F32)).astype(BF16)
    return jnp.dot(hi, b, preferred_element_type=F32) + jnp.dot(lo, b, preferred_element_type=F32)


def split_dot_right(a, b):
    hi = b.astype(BF16)
    lo = (b - hi.astype(F32)).astype(BF16)
    return jnp.dot(a, hi, preferred_element_type=F32) + jnp.dot(a, lo, preferred_element_type=F32)


def grid_of(shape, dim):
    return lax.broadcasted_iota(jnp.int32, shape, dim)


def mix_kernel(features, steps, proj_ref, total_ref, live_ref, base_ref, gain_ref, state_ref, *rest):
    gated_ref, final_ref = rest[-2], rest[-1]
    rows = proj_ref.shape[0]
    span = base_ref.shape[1]
    heads = span // HEAD
    tall = heads * steps
    inv = lax.rsqrt(jnp.sum(total_ref[...], axis=1, keepdims=True) / features + norm_eps)
    recept, keys, values, decay_pre, rate_pre, gate_pre = (
        proj_ref[:, i * span : (i + 1) * span] * inv for i in range(6)
    )
    live = live_ref[...][:, 0:1]
    seg = (grid_of((span, span), 0) // HEAD == grid_of((span, span), 1) // HEAD).astype(F32).astype(BF16)
    rb = grid_of((rows, rows), 0)
    cb = grid_of((rows, rows), 1)
    same = rb // steps == cb // steps
    lower = jnp.where(same & (cb <= rb), 1.0, 0.0).astype(BF16)
    whole = jnp.where(same, 1.0, 0.0).astype(BF16)
    unit = keys * lax.rsqrt(split_dot(keys * keys, seg) + key_eps)
    removal = unit * jax.nn.sigmoid(rate_pre) * live
    logd = -decay_scale * jax.nn.sigmoid(decay_pre + base_ref[...]) * live
    upto = split_dot_right(lower, logd)
    ends = jnp.exp(split_dot_right(whole, logd))
    back = jnp.exp(-upto)
    u_in = unit * jnp.exp(upto - logd)
    q_in = recept * jnp.exp(upto)
    r_out = removal * back
    k_out = keys * live * back
    r_end = r_out * ends
    k_end = k_out * ends
    scale_out = gain_ref[...] * jax.nn.sigmoid(gate_pre) * live

    mask = jnp.where(
        grid_of((tall, span), 0) // steps == grid_of((tall, span), 1) // HEAD, 1.0, 0.0
    )
    fold = jnp.where(
        grid_of((span, HEAD), 0) % HEAD == grid_of((span, HEAD), 1), 1.0, 0.0
    ).astype(BF16)
    tr = grid_of((tall, tall), 0)
    tc = grid_of((tall, tall), 1)
    strict_m = jnp.where(tc < tr, 1.0, 0.0)
    lower_m = jnp.where(tc <= tr, 1.0, 0.0)
    nt = (((1,), (1,)), ((), ()))
    tn = (((0,), (0,)), ((), ()))

    def exact(a, b):
        return jnp.dot(a, b, preferred_element_type=F32, precision=lax.Precision.HIGHEST)

    def quick(a, b, dims=(((1,), (0,)), ((), ()))):
        return lax.dot_general(a.astype(BF16), b.astype(BF16), dims, preferred_element_type=F32)

    for b in range(rows // steps):
        cut = slice(b * steps, (b + 1) * steps)

        def spread(a):
            return (jnp.concatenate([a[cut]] * heads, axis=0) * mask).astype(BF16)

        memory = state_ref[0, b]
        ask = jnp.concatenate([spread(u_in), spread(q_in)], axis=0)
        on_s = quick(ask, memory, nt)
        on_r = quick(ask, spread(r_out), nt)
        on_k = quick(ask, spread(k_out), nt)
        m1 = on_r[:tall] * strict_m
        m2 = on_k[:tall] * strict_m
        p_r = on_r[tall:] * lower_m
        p_k = on_k[tall:] * lower_m
        vals = jnp.dot(spread(values), fold, preferred_element_type=F32)
        seen = on_s[:tall] + quick(m2, vals)
        squared = exact(m1, m1)
        fourth = exact(squared, squared)
        seen = seen + exact(fourth, seen)
        seen = seen + exact(squared, seen)
        seen = seen - exact(m1, seen)
        read = on_s[tall:] + quick(p_k, vals) - quick(p_r, seen)
        final_ref[0, b] = (
            memory * ends[b * steps : b * steps + 1]
            + quick(vals, spread(k_end), tn)
            - quick(seen, spread(r_end), tn)
        )
        centered = read - jnp.mean(read, axis=1, keepdims=True)
        normed = centered * lax.rsqrt(
            jnp.mean(centered * centered, axis=1, keepdims=True) + group_eps
        )
        wide = jnp.concatenate([normed, normed], axis=1)
        wide = jnp.concatenate([wide] * (heads // 2), axis=1) * mask
        flat = wide[0:steps]
        for h in range(1, heads):
            flat = flat + wide[h * steps : (h + 1) * steps]
        gated_ref[cut, :] = (flat * scale_out[cut]).astype(BF16)


def mix(block, features, steps, proj, total, live, base, gain, states, earlier):
    rows = proj.shape[0]
    span = base.shape[1]
    _, held, size, _ = states.shape
    full = lambda shape: pl.BlockSpec(shape, lambda i: (0,) * len(shape))
    slab = pl.BlockSpec((1, held, size, span), lambda i: (block, 0, 0, 0))
    args = [proj, total, live, base, gain, states]
    in_specs = [full(a.shape) for a in args[:5]] + [slab]
    aliases = {}
    if earlier is not None:
        args.append(earlier)
        in_specs.append(pl.BlockSpec(memory_space=pl.ANY))
        aliases = {6: 1}
    return pl.pallas_call(
        functools.partial(mix_kernel, features, steps),
        grid=(1,),
        out_shape=(
            jax.ShapeDtypeStruct((rows, span), BF16),
            jax.ShapeDtypeStruct(states.shape, F32),
        ),
        in_specs=in_specs,
        out_specs=(full((rows, span)), slab),
        input_output_aliases=aliases,
        compiler_params=pltpu.CompilerParams(vmem_limit_bytes=48 * 1024 * 1024),
        name="mix%d" % block,
    )(*args)


def output_kernel(
    block, ntp, ndp, rows,
    gated_ref, x_ref, w_ref, out_ref,
    wbuf, gg, osend, orecv, wsem, gs_sem, gr_sem, os_sem, or_sem,
):
    here = x_ref.shape[0]
    tp = lax.axis_index("tp")
    dp = lax.axis_index("dp")
    load = pltpu.make_async_copy(w_ref.at[block], wbuf, wsem)
    load.start()
    gg[pl.ds(pl.multiple_of(dp * rows, rows), rows), :] = gated_ref[...]
    greet(
        [("dp", lax.rem(dp + k, ndp)) for k in range(1, ndp)]
        + [("tp", lax.rem(tp + k, ntp)) for k in range(1, ntp)]
    )
    sends = []
    for k in range(1, ndp):
        at = gg.at[pl.ds(pl.multiple_of(dp * rows, rows), rows), :]
        cp = remote(gated_ref, at, gs_sem.at[k], gr_sem.at[k], "dp", lax.rem(dp + k, ndp))
        cp.start()
        sends.append(cp)
    for k in range(1, ndp):
        src = lax.rem(dp + ndp - k, ndp)
        at = gg.at[pl.ds(pl.multiple_of(src * rows, rows), rows), :]
        remote(gated_ref, at, gs_sem.at[k], gr_sem.at[k], "dp", src).wait_recv()
    load.wait()

    def partial_of(peer):
        take = gg[pl.ds(pl.multiple_of(peer * here, here), here), :]
        return jnp.dot(take, wbuf[...], preferred_element_type=F32)

    def copy_o(k):
        return remote(
            osend.at[k], orecv.at[k], os_sem.at[k], or_sem.at[k], "tp", lax.rem(tp + k, ntp)
        )

    def give(k, carry):
        osend[k] = partial_of(lax.rem(tp + k, ntp)).astype(BF16)
        copy_o(k).start()
        return carry

    lax.fori_loop(1, ntp, give, 0)
    out_ref[...] = x_ref[...].astype(F32) + partial_of(tp)

    def take(k, carry):
        copy_o(k).wait_recv()
        out_ref[...] += orecv[k].astype(F32)
        copy_o(k).wait_send()
        return carry

    lax.fori_loop(1, ntp, take, 0)
    for cp in sends:
        cp.wait_send()


def output(block, ntp, ndp, gated, x, w_out, ident):
    rows, span = gated.shape
    here, depth = x.shape
    dma = pltpu.SemaphoreType.DMA
    vmem = pl.BlockSpec(memory_space=pltpu.VMEM)
    return pl.pallas_call(
        functools.partial(output_kernel, block, ntp, ndp, rows),
        out_shape=jax.ShapeDtypeStruct((here, depth), F32),
        in_specs=[vmem, vmem, pl.BlockSpec(memory_space=pl.ANY)],
        out_specs=vmem,
        scratch_shapes=[
            pltpu.VMEM((span, depth), BF16),
            pltpu.VMEM((ndp * rows, span), BF16),
            pltpu.VMEM((ntp, here, depth), BF16),
            pltpu.VMEM((ntp, here, depth), BF16),
            dma,
            dma((ndp,)), dma((ndp,)), dma((ntp,)), dma((ntp,)),
        ],
        compiler_params=pltpu.CompilerParams(
            collective_id=ident, has_side_effects=True, vmem_limit_bytes=48 * 1024 * 1024
        ),
        name="output%d" % block,
    )(gated, x, w_out)


def body(
    ntp, ndp,
    tokens, lengths, norm_gain,
    w_recept, w_key, w_value, w_decay, w_rate, w_gate,
    w_out, decay_base, out_gain, states,
):
    seqs, steps, depth = tokens.shape
    held = states.shape[1]
    rows = held * steps
    features = depth * ndp
    first_row = lax.axis_index("dp") * held
    held_lengths = lax.dynamic_slice_in_dim(lengths, first_row, held, 0)
    live = jnp.arange(steps, dtype=jnp.int32)[None, :] < held_lengths[:, None]
    live = jnp.broadcast_to(live.astype(F32).reshape(rows, 1), (rows, LANES))
    current = tokens.reshape(seqs * steps, depth)
    weights = (w_recept, w_key, w_value, w_decay, w_rate, w_gate)
    finals = None
    for block in range(BLOCKS):
        proj, total = project(
            block, ntp, ndp, rows, current, norm_gain[block : block + 1], weights, 2 * block
        )
        gated, finals = mix(
            block, features, steps, proj, total, live,
            decay_base[block : block + 1], out_gain[block : block + 1], states, finals,
        )
        current = output(block, ntp, ndp, gated, current, w_out, 2 * block + 1)
    return (current.reshape(seqs, steps, depth), finals)


def solution(mesh):
    in_specs = (
        P(("grp", "tp"), None, "dp"),
        P("grp"),
        P(None, "dp"),
        P(None, "dp", "tp"),
        P(None, "dp", "tp"),
        P(None, "dp", "tp"),
        P(None, "dp", "tp"),
        P(None, "dp", "tp"),
        P(None, "dp", "tp"),
        P(None, "tp", "dp"),
        P(None, "tp"),
        P(None, "tp"),
        P(None, ("grp", "dp"), None, "tp"),
    )
    out_specs = (P(("grp", "tp"), None, "dp"), P(None, ("grp", "dp"), None, "tp"))
    run = functools.partial(body, mesh.shape["tp"], mesh.shape["dp"])
    return jax.shard_map(run, mesh=mesh, in_specs=in_specs, out_specs=out_specs, check_vma=False)
```

```python
import functools

import jax
import jax.numpy as jnp
from jax import lax
from jax.experimental import pallas as pl
from jax.experimental.pallas import tpu as pltpu
from jax.sharding import PartitionSpec as P

HEAD = 64
BLOCKS = 2
LANES = 128
CORES = 2

group_eps = 0.00064
norm_eps = 1e-06
key_eps = 1e-06
decay_scale = 0.606531
MESH = pl.DeviceIdType.MESH
F32 = jnp.float32
BF16 = jnp.bfloat16


def remote(src, dst, send, recv, axis, peer):
    return pltpu.make_async_remote_copy(
        src_ref=src,
        dst_ref=dst,
        send_sem=send,
        recv_sem=recv,
        device_id={axis: peer},
        device_id_type=MESH,
    )


def greet(peers):
    barrier = pltpu.get_barrier_semaphore()
    for axis, peer in peers:
        pl.semaphore_signal(barrier, inc=1, device_id={axis: peer}, device_id_type=MESH)
    pl.semaphore_wait(barrier, len(peers))


def project_kernel(
    block, ntp, ndp, rows, width,
    x_ref, gain_ref, w0, w1, w2, w3, w4, w5,
    out_ref, total_ref,
    wbuf, xg, sqg, part, recv_a, send_b, recv_b, sq_a, sq_ra, sq_b, sq_rb,
    wsem, xs_sem, xr_sem, ss_sem, sr_sem, as_sem, ar_sem, bs_sem, br_sem,
    qas_sem, qar_sem, qbs_sem, qbr_sem,
):
    weights = (w0, w1, w2, w3, w4, w5)
    chunks, depth, _ = wbuf.shape
    halves = chunks // 6
    nx = ndp // CORES
    tp = lax.axis_index("tp")
    dp = lax.axis_index("dp")
    core = lax.rem(dp, CORES)
    xpos = dp // CORES
    partner = dp + 1 - 2 * core

    def load(c):
        return pltpu.make_async_copy(
            weights[c // halves].at[block, :, pl.ds((c % halves) * width, width)],
            wbuf.at[c],
            wsem.at[c],
        )

    for c in range(chunks):
        load(c).start()
    x = x_ref[...].astype(F32)
    xg[tp] = (x * gain_ref[block : block + 1, :]).astype(BF16)
    sq = x * x
    acc = sq[:, 0:LANES]
    for k in range(1, depth // LANES):
        acc = acc + sq[:, k * LANES : (k + 1) * LANES]
    sqg[tp] = acc
    peers = [("tp", lax.rem(tp + k, ntp)) for k in range(1, ntp)]
    peers += [("dp", partner)]
    peers += [("dp", CORES * lax.rem(xpos + k, nx) + core) for k in range(1, nx)]
    greet(peers)

    gathers = []
    for k in range(1, ntp):
        peer = lax.rem(tp + k, ntp)
        cp = remote(xg.at[tp], xg.at[tp], xs_sem.at[k], xr_sem.at[k], "tp", peer)
        cq = remote(sqg.at[tp], sqg.at[tp], ss_sem.at[k], sr_sem.at[k], "tp", peer)
        cp.start()
        cq.start()
        gathers += [cp, cq]
    for k in range(1, ntp):
        src = lax.rem(tp + ntp - k, ntp)
        remote(xg.at[src], xg.at[src], xs_sem.at[k], xr_sem.at[k], "tp", src).wait_recv()
        remote(sqg.at[src], sqg.at[src], ss_sem.at[k], sr_sem.at[k], "tp", src).wait_recv()

    sq_all = sqg[...].reshape(ndp, rows, LANES)
    part_sq = [sq_all[d] for d in range(ndp)]

    def pick(parts, x_at, which):
        return jnp.where(which == 0, parts[CORES * x_at], parts[CORES * x_at + 1])

    for xd in range(nx):
        sq_a[xd] = pick(part_sq, xd, 1 - core)
        sq_b[xd] = pick(part_sq, xd, core)
    copy_qa = remote(sq_a, sq_ra, qas_sem, qar_sem, "dp", partner)
    copy_qa.start()

    def copy_a(c):
        return remote(part.at[c, 1 - core], recv_a.at[c], as_sem.at[c], ar_sem.at[c], "dp", partner)

    def copy_b(c, k):
        xd = lax.rem(xpos + k, nx)
        return remote(
            send_b.at[c, k], recv_b.at[c, k], bs_sem.at[c, k], br_sem.at[c, k],
            "dp", CORES * xd + core,
        )

    def stage_b(c):
        copy_a(c).wait_recv()
        for k in range(1, nx):
            xd = lax.rem(xpos + k, nx)
            send_b[c, k] = (part[c, core, xd] + recv_a[c, xd]).astype(BF16)
            copy_b(c, k).start()

    def first(c, carry):
        pltpu.make_async_copy(wbuf.at[c], wbuf.at[c], wsem.at[c]).wait()
        res = jnp.dot(
            xg[...].reshape(ndp * rows, depth), wbuf[c], preferred_element_type=F32
        )
        for d in range(ndp):
            part[c, d % CORES, d // CORES] = res[d * rows : (d + 1) * rows]
        copy_a(c).start()

        @pl.when(c > 0)
        def _():
            stage_b(c - 1)

        return carry

    lax.fori_loop(0, chunks, first, 0)
    copy_qa.wait_recv()
    for xd in range(nx):
        sq_b[xd] = sq_b[xd] + sq_ra[xd]
    qb = []
    for k in range(1, nx):
        xd = lax.rem(xpos + k, nx)
        cp = remote(
            sq_b.at[xd], sq_rb.at[k], qbs_sem.at[k], qbr_sem.at[k], "dp", CORES * xd + core
        )
        cp.start()
        qb.append(cp)
    stage_b(chunks - 1)

    def last(c, carry):
        own = part[c, core, xpos] + recv_a[c, xpos]
        for k in range(1, nx):
            copy_b(c, k).wait_recv()
            own = own + recv_b[c, k].astype(F32)
        out_ref[:, pl.ds(pl.multiple_of(c * width, width), width)] = own
        copy_a(c).wait_send()
        for k in range(1, nx):
            copy_b(c, k).wait_send()
        return carry

    lax.fori_loop(0, chunks, last, 0)
    total = sq_b[xpos]
    for k in range(1, nx):
        qb[k - 1].wait_recv()
        total = total + sq_rb[k]
    total_ref[...] = total
    copy_qa.wait_send()
    for cp in qb:
        cp.wait_send()
    for cp in gathers:
        cp.wait_send()


def project(block, ntp, ndp, rows, x, gain, weights, ident):
    here, depth = x.shape
    span = weights[0].shape[2]
    width = min(256, span)
    chunks = 6 * span // width
    nx = ndp // CORES
    dma = pltpu.SemaphoreType.DMA
    vmem = pl.BlockSpec(memory_space=pltpu.VMEM)
    hbm = pl.BlockSpec(memory_space=pltpu.HBM)
    return pl.pallas_call(
        functools.partial(project_kernel, block, ntp, ndp, rows, width),
        out_shape=(
            jax.ShapeDtypeStruct((rows, 6 * span), F32),
            jax.ShapeDtypeStruct((rows, LANES), F32),
        ),
        in_specs=[vmem, vmem] + [hbm] * 6,
        out_specs=(vmem, vmem),
        scratch_shapes=[
            pltpu.VMEM((chunks, depth, width), BF16),
            pltpu.VMEM((ntp, here, depth), BF16),
            pltpu.VMEM((ntp, here, LANES), F32),
            pltpu.VMEM((chunks, CORES, nx, rows, width), F32),
            pltpu.VMEM((chunks, nx, rows, width), F32),
            pltpu.VMEM((chunks, nx, rows, width), BF16),
            pltpu.VMEM((chunks, nx, rows, width), BF16),
            pltpu.VMEM((nx, rows, LANES), F32),
            pltpu.VMEM((nx, rows, LANES), F32),
            pltpu.VMEM((nx, rows, LANES), F32),
            pltpu.VMEM((nx, rows, LANES), F32),
            dma((chunks,)),
            dma((ntp,)), dma((ntp,)), dma((ntp,)), dma((ntp,)),
            dma((chunks,)), dma((chunks,)),
            dma((chunks, nx)), dma((chunks, nx)),
            dma, dma, dma((nx,)), dma((nx,)),
        ],
        compiler_params=pltpu.CompilerParams(
            collective_id=ident, has_side_effects=True, vmem_limit_bytes=65500000
        ),
        name="project%d" % block,
    )(x, gain, *weights)


def halves(a):
    hi = a.astype(BF16)
    return hi, (a - hi.astype(F32)).astype(BF16)


def split_dot(a, b):
    hi, lo = halves(a)
    return jnp.dot(hi, b, preferred_element_type=F32) + jnp.dot(lo, b, preferred_element_type=F32)


def split_dot_right(a, b):
    hi, lo = halves(b)
    return jnp.dot(a, hi, preferred_element_type=F32) + jnp.dot(a, lo, preferred_element_type=F32)


def grid_of(shape, dim):
    return lax.broadcasted_iota(jnp.int32, shape, dim)


def mix_kernel(block, features, steps, proj_ref, total_ref, live_ref, base_ref, gain_ref, state_ref, *rest):
    gated_ref, final_ref = rest[-2], rest[-1]
    rows = proj_ref.shape[0]
    span = base_ref.shape[1]
    heads = span // HEAD
    tall = heads * steps
    inv = lax.rsqrt(jnp.sum(total_ref[...], axis=1, keepdims=True) / features + norm_eps)
    recept, keys, values, decay_pre, rate_pre, gate_pre = (
        proj_ref[:, i * span : (i + 1) * span] * inv for i in range(6)
    )
    live = live_ref[...][:, 0:1]
    seg = (grid_of((span, span), 0) // HEAD == grid_of((span, span), 1) // HEAD).astype(F32).astype(BF16)
    rb = grid_of((rows, rows), 0)
    cb = grid_of((rows, rows), 1)
    same = rb // steps == cb // steps
    lower = jnp.where(same & (cb <= rb), 1.0, 0.0).astype(BF16)
    whole = jnp.where(same, 1.0, 0.0).astype(BF16)
    unit = keys * lax.rsqrt(split_dot(keys * keys, seg) + key_eps)
    removal = unit * jax.nn.sigmoid(rate_pre) * live
    logd = -decay_scale * jax.nn.sigmoid(decay_pre + base_ref[block : block + 1, :]) * live
    upto = split_dot_right(lower, logd)
    ends = jnp.exp(split_dot_right(whole, logd))
    back = jnp.exp(-upto)
    u_in = unit * jnp.exp(upto - logd)
    q_in = recept * jnp.exp(upto)
    r_out = removal * back
    k_out = keys * live * back
    r_end = r_out * ends
    k_end = k_out * ends
    scale_out = gain_ref[block : block + 1, :] * jax.nn.sigmoid(gate_pre) * live

    mask = jnp.where(
        grid_of((tall, span), 0) // steps == grid_of((tall, span), 1) // HEAD, 1.0, 0.0
    )
    fold = jnp.where(
        grid_of((span, HEAD), 0) % HEAD == grid_of((span, HEAD), 1), 1.0, 0.0
    ).astype(BF16)
    tr = grid_of((tall, tall), 0)
    tc = grid_of((tall, tall), 1)
    strict_m = jnp.where(tc < tr, 1.0, 0.0)
    lower_m = jnp.where(tc <= tr, 1.0, 0.0)
    nt = (((1,), (1,)), ((), ()))
    tn = (((0,), (0,)), ((), ()))

    def exact(a, b):
        return jnp.dot(a, b, preferred_element_type=F32, precision=lax.Precision.HIGHEST)

    def quick(a, b, dims=(((1,), (0,)), ((), ()))):
        return lax.dot_general(a.astype(BF16), b.astype(BF16), dims, preferred_element_type=F32)

    for b in range(rows // steps):
        cut = slice(b * steps, (b + 1) * steps)

        def spread(a):
            return jnp.concatenate([a[cut]] * heads, axis=0) * mask

        memory = state_ref[0, b]
        m_hi, m_lo = halves(memory)
        a_hi, a_lo = halves(jnp.concatenate([spread(u_in), spread(q_in)], axis=0))
        k_hi, k_lo = halves(spread(k_out))
        v_all = jnp.concatenate(halves(spread(values)), axis=0)
        both = quick(a_hi, jnp.concatenate([m_hi, m_lo, k_hi, k_lo], axis=0), nt)
        tail = quick(a_lo, jnp.concatenate([m_hi, k_hi], axis=0), nt)
        on_r = quick(a_hi, spread(r_out), nt)
        at = 2 * HEAD
        on_s = both[:, :HEAD] + both[:, HEAD:at] + tail[:, :HEAD]
        on_k = both[:, at : at + tall] + both[:, at + tall :] + tail[:, HEAD:]
        m1 = on_r[:tall] * strict_m
        m2 = on_k[:tall] * strict_m
        p_r = on_r[tall:] * lower_m
        p_k = on_k[tall:] * lower_m
        folded = quick(v_all, fold)
        vals = folded[:tall] + folded[tall:]
        seen = on_s[:tall] + quick(m2, vals)
        squared = exact(m1, m1)
        fourth = exact(squared, squared)
        seen = seen + exact(fourth, seen)
        seen = seen + exact(squared, seen)
        seen = seen - exact(m1, seen)
        read = on_s[tall:] + exact(p_k, vals) - quick(p_r, seen)
        v_hi, v_lo = halves(vals)
        e_hi, e_lo = halves(spread(k_end))
        left = jnp.concatenate([v_hi, v_lo, v_hi, (-seen).astype(BF16)], axis=0)
        right = jnp.concatenate([e_hi, e_hi, e_lo, spread(r_end).astype(BF16)], axis=0)
        final_ref[0, b] = memory * ends[b * steps : b * steps + 1] + quick(left, right, tn)
        centered = read - jnp.mean(read, axis=1, keepdims=True)
        normed = centered * lax.rsqrt(
            jnp.mean(centered * centered, axis=1, keepdims=True) + group_eps
        )
        wide = jnp.concatenate([normed, normed], axis=1)
        wide = jnp.concatenate([wide] * (heads // 2), axis=1) * mask
        flat = wide[0:steps]
        for h in range(1, heads):
            flat = flat + wide[h * steps : (h + 1) * steps]
        gated_ref[cut, :] = (flat * scale_out[cut]).astype(BF16)


def mix(block, features, steps, proj, total, live, base, gain, states, earlier):
    rows = proj.shape[0]
    span = base.shape[1]
    _, held, size, _ = states.shape
    full = lambda shape: pl.BlockSpec(shape, lambda i: (0,) * len(shape))
    slab = pl.BlockSpec((1, held, size, span), lambda i: (block, 0, 0, 0))
    args = [proj, total, live, base, gain, states]
    in_specs = [full(a.shape) for a in args[:5]] + [slab]
    aliases = {}
    if earlier is not None:
        args.append(earlier)
        in_specs.append(pl.BlockSpec(memory_space=pl.ANY))
        aliases = {6: 1}
    return pl.pallas_call(
        functools.partial(mix_kernel, block, features, steps),
        grid=(1,),
        out_shape=(
            jax.ShapeDtypeStruct((rows, span), BF16),
            jax.ShapeDtypeStruct(states.shape, F32),
        ),
        in_specs=in_specs,
        out_specs=(full((rows, span)), slab),
        input_output_aliases=aliases,
        compiler_params=pltpu.CompilerParams(vmem_limit_bytes=48 * 1024 * 1024),
        name="mix%d" % block,
    )(*args)


def output_kernel(
    block, ntp, ndp, rows,
    gated_ref, x_ref, w_ref, out_ref,
    wbuf, gg, osend, orecv, wsem, gs_sem, gr_sem, os_sem, or_sem,
):
    here = x_ref.shape[0]
    tp = lax.axis_index("tp")
    dp = lax.axis_index("dp")
    load = pltpu.make_async_copy(w_ref.at[block], wbuf, wsem)
    load.start()
    gg[pl.ds(pl.multiple_of(dp * rows, rows), rows), :] = gated_ref[...]
    greet(
        [("dp", lax.rem(dp + k, ndp)) for k in range(1, ndp)]
        + [("tp", lax.rem(tp + k, ntp)) for k in range(1, ntp)]
    )
    sends = []
    for k in range(1, ndp):
        at = gg.at[pl.ds(pl.multiple_of(dp * rows, rows), rows), :]
        cp = remote(gated_ref, at, gs_sem.at[k], gr_sem.at[k], "dp", lax.rem(dp + k, ndp))
        cp.start()
        sends.append(cp)
    for k in range(1, ndp):
        src = lax.rem(dp + ndp - k, ndp)
        at = gg.at[pl.ds(pl.multiple_of(src * rows, rows), rows), :]
        remote(gated_ref, at, gs_sem.at[k], gr_sem.at[k], "dp", src).wait_recv()
    load.wait()

    def partial_of(peer):
        take = gg[pl.ds(pl.multiple_of(peer * here, here), here), :]
        return jnp.dot(take, wbuf[...], preferred_element_type=F32)

    def copy_o(k):
        return remote(
            osend.at[k], orecv.at[k], os_sem.at[k], or_sem.at[k], "tp", lax.rem(tp + k, ntp)
        )

    def give(k, carry):
        osend[k] = partial_of(lax.rem(tp + k, ntp)).astype(BF16)
        copy_o(k).start()
        return carry

    lax.fori_loop(1, ntp, give, 0)
    out_ref[...] = x_ref[...].astype(F32) + partial_of(tp)

    def take(k, carry):
        copy_o(k).wait_recv()
        out_ref[...] += orecv[k].astype(F32)
        copy_o(k).wait_send()
        return carry

    lax.fori_loop(1, ntp, take, 0)
    for cp in sends:
        cp.wait_send()


def output(block, ntp, ndp, gated, x, w_out, ident):
    rows, span = gated.shape
    here, depth = x.shape
    dma = pltpu.SemaphoreType.DMA
    vmem = pl.BlockSpec(memory_space=pltpu.VMEM)
    return pl.pallas_call(
        functools.partial(output_kernel, block, ntp, ndp, rows),
        out_shape=jax.ShapeDtypeStruct((here, depth), F32),
        in_specs=[vmem, vmem, pl.BlockSpec(memory_space=pltpu.HBM)],
        out_specs=vmem,
        scratch_shapes=[
            pltpu.VMEM((span, depth), BF16),
            pltpu.VMEM((ndp * rows, span), BF16),
            pltpu.VMEM((ntp, here, depth), BF16),
            pltpu.VMEM((ntp, here, depth), BF16),
            dma,
            dma((ndp,)), dma((ndp,)), dma((ntp,)), dma((ntp,)),
        ],
        compiler_params=pltpu.CompilerParams(
            collective_id=ident, has_side_effects=True, vmem_limit_bytes=48 * 1024 * 1024
        ),
        name="output%d" % block,
    )(gated, x, w_out)


def body(
    ntp, ndp,
    tokens, lengths, norm_gain,
    w_recept, w_key, w_value, w_decay, w_rate, w_gate,
    w_out, decay_base, out_gain, states,
):
    seqs, steps, depth = tokens.shape
    held = states.shape[1]
    rows = held * steps
    features = depth * ndp
    first_row = lax.axis_index("dp") * held
    held_lengths = lax.dynamic_slice_in_dim(lengths, first_row, held, 0)
    live = jnp.arange(steps, dtype=jnp.int32)[None, :] < held_lengths[:, None]
    live = jnp.broadcast_to(live.astype(F32).reshape(rows, 1), (rows, LANES))
    current = tokens.reshape(seqs * steps, depth)
    weights = (w_recept, w_key, w_value, w_decay, w_rate, w_gate)
    finals = None
    for block in range(BLOCKS):
        proj, total = project(
            block, ntp, ndp, rows, current, norm_gain, weights, 2 * block
        )
        gated, finals = mix(
            block, features, steps, proj, total, live,
            decay_base, out_gain, states, finals,
        )
        current = output(block, ntp, ndp, gated, current, w_out, 2 * block + 1)
    return (current.reshape(seqs, steps, depth), finals)


def solution(mesh):
    in_specs = (
        P(("grp", "tp"), None, "dp"),
        P("grp"),
        P(None, "dp"),
        P(None, "dp", "tp"),
        P(None, "dp", "tp"),
        P(None, "dp", "tp"),
        P(None, "dp", "tp"),
        P(None, "dp", "tp"),
        P(None, "dp", "tp"),
        P(None, "tp", "dp"),
        P(None, "tp"),
        P(None, "tp"),
        P(None, ("grp", "dp"), None, "tp"),
    )
    out_specs = (P(("grp", "tp"), None, "dp"), P(None, ("grp", "dp"), None, "tp"))
    run = functools.partial(body, mesh.shape["tp"], mesh.shape["dp"])
    return jax.shard_map(run, mesh=mesh, in_specs=in_specs, out_specs=out_specs, check_vma=False)
```
